128 devices in a mesh: rep: 2 (over z_hi), fs: 32 (over z_lo, y, x), tp: 2 (over core).
Axes of the slice: x: 4, y: 4, z: 4 (z_hi: 2, z_lo: 2; z = z_hi * 2 + z_lo), core: 2. Of those that a mesh axis runs over, the one named last changes fastest.
Arguments:
- tokens: bfloat16 [256, 64, 2048], P('tp', ('rep', 'fs')), may hold values from -6 to 6
- mix_gain: float32 [2048], replicated, may hold values from 0.1 to 1.9
- value_weight: bfloat16 [2048, 1024], P('fs', 'tp'), may hold values from -0.125 to 0.125
- gate_weight: bfloat16 [2048, 1024], P('fs', 'tp'), may hold values from -0.125 to 0.125
- conv_taps: float32 [31, 1024], P(None, 'tp'), may hold values from -1 to 1
- head_gain: float32 [1024], P('tp'), may hold values from 0.1 to 1.9
- out_weight: bfloat16 [1024, 2048], P('tp', 'fs'), may hold values from -0.1875 to 0.1875
- ffn_gain: float32 [2048], replicated, may hold values from 0.1 to 1.9
- ffn_gate_weight: bfloat16 [2048, 3072], P('fs', 'tp'), may hold values from -0.125 to 0.125
- ffn_up_weight: bfloat16 [2048, 3072], P('fs', 'tp'), may hold values from -0.125 to 0.125
- down_weight: bfloat16 [3072, 2048], P('tp', 'fs'), may hold values from -0.109375 to 0.109375
Outputs:
- layer_out: bfloat16 [256, 64, 2048], P('tp', ('rep', 'fs'))
The draws below stay inside these ranges and needn't reach their ends.
All inputs are finite; a program needn't handle non-finite values.
Results may differ from the reference program's by a relative error of at most 0.012.
Values may be sent and summed in bfloat16 or wider, within the bound.
No kernel may reach another device: no remote copies, remote signals or barrier semaphores. Data moves between devices by JAX's collectives and lax.ppermute only.
A program may use at most 128 MiB of HBM per device.

```python
import jax
import jax.numpy as jnp
from jax import lax

D = 2048
HEADS = 8
HEAD_DIM = 128
FF = 3072
KW = 31
LEN = 256
SEQ_DEV = 1
CH = 1024
BATCH = 64
N_TP = 2


def block_levels(stream_key, dims, pieces, low, high):
    loudness = 1.0
    for axis_at, parts in pieces:
        heights = jax.random.uniform(jax.random.fold_in(jax.random.fold_in(stream_key, 6), axis_at), (parts,), jnp.float32, low / len(pieces), high / len(pieces))
        loudness = loudness * jnp.repeat(jnp.exp(heights), dims[axis_at] // parts).reshape((-1,) + (1,) * (len(dims) - 1 - axis_at))
    return loudness


def centred(stream_key, extent, deviation, bound, shards=(), kind=jnp.bfloat16):
    gain = block_levels(stream_key, extent, shards, -0.22, 0.18) if shards else 1.0
    drawn = jax.random.normal(stream_key, extent, jnp.float32) * deviation * gain
    return jnp.minimum(jnp.maximum(drawn, -bound), bound).astype(kind)


def setup_inputs(seed: int = 0) -> dict:
    keys = jax.random.split(jax.random.key(seed), 12)
    return {
        "tokens": centred(keys[0], (LEN, BATCH, D), 1.0, 6.0, ((0, 2), (1, 64))),
        "mix_gain": jnp.clip(1.0 + 0.18 * jax.random.normal(keys[1], (D,), jnp.float32), 0.1, 1.9),
        "value_weight": centred(keys[2], (D, CH), D ** -0.5, 0.125, ((0, 32), (1, 2))),
        "gate_weight": centred(keys[3], (D, CH), D ** -0.5, 0.125, ((0, 32), (1, 2))),
        "conv_taps": centred(keys[4], (KW, CH), KW ** -0.5, 1.0, ((1, 2),), jnp.float32),
        "head_gain": jnp.clip(1.0 + 0.18 * jax.random.normal(keys[5], (CH,), jnp.float32), 0.1, 1.9),
        "out_weight": centred(keys[6], (CH, D), CH ** -0.5, 0.1875, ((0, 2), (1, 32))),
        "ffn_gain": jnp.clip(1.0 + 0.18 * jax.random.normal(keys[7], (D,), jnp.float32), 0.1, 1.9),
        "ffn_gate_weight": centred(keys[8], (D, FF), D ** -0.5, 0.125, ((0, 32), (1, 2))),
        "ffn_up_weight": centred(keys[9], (D, FF), D ** -0.5, 0.125, ((0, 32), (1, 2))),
        "down_weight": centred(keys[10], (FF, D), FF ** -0.5, 0.109375, ((0, 2), (1, 32))),
    }


norm_eps = 1e-06
group_eps = 1e-05

def rms_scale(matrix, scales):
    return matrix * lax.rsqrt(lax.optimization_barrier(jnp.mean(matrix * matrix, axis=-1, keepdims=True)) + norm_eps) * scales

def split_sum(activated, weights, block_width):
    summed = jnp.zeros((activated.shape[0], weights.shape[1]), jnp.float32)
    for block_idx in range(N_TP):
        lower = block_idx * block_width
        partial_value = jnp.dot(activated[:, lower:lower + block_width], weights[lower:lower + block_width], preferred_element_type=jnp.float32).astype(jnp.bfloat16)
        partial_value = lax.optimization_barrier(partial_value)
        summed = summed + partial_value.astype(jnp.float32)
    return summed

def reference(tokens, mix_gain, value_weight, gate_weight, conv_taps, head_gain, out_weight, ffn_gain, ffn_gate_weight, ffn_up_weight, down_weight):

    def sequence_block(inputs):
        seq_count = inputs.shape[1]
        residual = inputs.reshape(-1, D).astype(jnp.float32)
        normed = rms_scale(residual, mix_gain).astype(jnp.bfloat16)
        value_rows = jnp.dot(normed, value_weight, preferred_element_type=jnp.float32)
        gate_rows = jnp.dot(normed, gate_weight, preferred_element_type=jnp.float32)
        glu_rows = (value_rows * jax.nn.sigmoid(gate_rows)).astype(jnp.bfloat16).reshape(LEN, seq_count, CH)
        conved = lax.conv_general_dilated(glu_rows.astype(jnp.float32), conv_taps[:, None, :], (1,), [(KW // 2, KW // 2)], dimension_numbers=('WNC', 'WIO', 'WNC'), feature_group_count=CH, precision=lax.Precision.HIGHEST)
        grouped = conved.reshape(LEN, seq_count, HEADS, HEAD_DIM)
        head_mean = lax.optimization_barrier(jnp.mean(grouped, axis=-1, keepdims=True))
        head_var = lax.optimization_barrier(jnp.mean(jnp.square(grouped - head_mean), axis=-1, keepdims=True))
        scaled = (grouped - head_mean) * lax.rsqrt(head_var + group_eps) * head_gain.reshape(HEADS, HEAD_DIM)
        activated = jax.nn.silu(scaled).astype(jnp.bfloat16).reshape(-1, CH)
        mixed_rows = split_sum(activated, out_weight, CH // N_TP)
        middle = (residual + mixed_rows).astype(jnp.bfloat16)
        middle_f = middle.astype(jnp.float32)
        normed_ffn = rms_scale(middle_f, ffn_gain).astype(jnp.bfloat16)
        gate_part = jnp.dot(normed_ffn, ffn_gate_weight, preferred_element_type=jnp.float32)
        up_part = jnp.dot(normed_ffn, ffn_up_weight, preferred_element_type=jnp.float32)
        hidden = (jax.nn.silu(gate_part) * up_part).astype(jnp.bfloat16)
        fed_rows = split_sum(hidden, down_weight, FF // N_TP)
        return (middle_f + fed_rows).astype(jnp.bfloat16).reshape(inputs.shape)
    blocks = tokens.reshape(LEN, BATCH // SEQ_DEV, SEQ_DEV, D).transpose(1, 0, 2, 3)
    results = lax.map(sequence_block, blocks)
    return results.transpose(1, 0, 2, 3).reshape(LEN, BATCH, D)
```

```python
import jax
import jax.numpy as jnp
from jax import lax
from jax.sharding import Mesh, PartitionSpec as P


HEAD_DIM = 128
HALO = 16
norm_eps = 1e-06
group_eps = 1e-05

Z = ("zh", "zl")
FS = ("zl", "y", "x")
SHIFTS = (1, 3, 2)
f32 = jnp.float32
bf16 = jnp.bfloat16


def swap_cores(value):
    return lax.ppermute(value, "tp", [(0, 1), (1, 0)])


def shift_z(value, by):
    return lax.ppermute(value, Z, [(i, (i + by) % 4) for i in range(4)])


def quarters_for_pair(weight):
    half = weight.shape[1] // 2
    mine = lax.dynamic_slice_in_dim(weight, lax.axis_index("zh") * half, half, axis=1)
    return jnp.moveaxis(mine.reshape(weight.shape[0], 2, half // 2), 1, 0)


def gathered(blocks):
    rows, cols = blocks.shape[-2:]
    spread = jnp.broadcast_to(blocks[:, None], (blocks.shape[0], 32 // blocks.shape[0], rows, cols))
    out = lax.all_to_all(spread.reshape(32, rows, cols), FS, 0, 0, tiled=True)
    return out.reshape(32 * rows, cols)


def rms_scale(matrix, scales):
    return matrix * lax.rsqrt(jnp.mean(matrix * matrix, axis=-1, keepdims=True) + norm_eps) * scales


def dot(a, b):
    return jnp.dot(a, b, preferred_element_type=f32)


def dot_t(a, b):
    return lax.dot_general(a, b, (((1,), (1,)), ((), ())), preferred_element_type=f32)


def body(
    tokens,
    mix_gain,
    value_weight,
    gate_weight,
    conv_taps,
    head_gain,
    out_weight,
    ffn_gain,
    ffn_gate_weight,
    ffn_up_weight,
    down_weight,
):
    rows, _, width = tokens.shape
    z = 2 * lax.axis_index("zh") + lax.axis_index("zl")
    tp = lax.axis_index("tp")
    ch = value_weight.shape[1] // 4

    residual = tokens.reshape(rows, width).astype(f32)
    normed = rms_scale(residual, mix_gain).astype(bf16)
    normed_all = [normed] + [shift_z(normed, d) for d in SHIFTS]

    vg = gathered(jnp.concatenate([quarters_for_pair(value_weight), quarters_for_pair(gate_weight)], axis=2))
    vg_other = swap_cores(vg)
    small = jnp.concatenate([conv_taps, head_gain[None]], axis=0)
    small = lax.dynamic_slice_in_dim(small, z * ch, ch, axis=1)
    small_other = swap_cores(small)
    small = jnp.concatenate([small, small_other], axis=1)
    outw = gathered(out_weight.T[None])
    outw_other = swap_cores(outw)
    gu = gathered(
        jnp.concatenate([quarters_for_pair(ffn_gate_weight), quarters_for_pair(ffn_up_weight)], axis=2)
    )
    gu_other = swap_cores(gu)
    down = gathered(quarters_for_pair(down_weight.T))
    down_other = swap_cores(down)

    stacked = jnp.concatenate(normed_all, axis=0)

    def glu_of(w):
        both = dot(stacked, w)
        return (both[:, :ch] * jax.nn.sigmoid(both[:, ch:])).astype(bf16)

    glu = jnp.concatenate([glu_of(vg), glu_of(vg_other)], axis=1).reshape(4, rows, 2 * ch)
    edge = lax.dynamic_slice_in_dim(glu, jnp.where(tp == 0, rows - HALO, 0), HALO, axis=1)
    edge = swap_cores(edge)
    edge = jnp.concatenate([edge[..., ch:], edge[..., :ch]], axis=-1)
    nothing = jnp.zeros_like(edge)
    padded = jnp.concatenate(
        [jnp.where(tp == 1, edge, nothing), glu, jnp.where(tp == 0, edge, nothing)], axis=1
    ).astype(f32)
    taps = small[:-1]
    width_k = taps.shape[0]
    conved = jnp.zeros((4, rows, 2 * ch), f32)
    for k in range(width_k):
        conved = conved + taps[k] * lax.slice_in_dim(padded, k + 1, k + 1 + rows, axis=1)
    grouped = conved.reshape(4, rows, 2, ch)
    mean = jnp.mean(grouped, axis=-1, keepdims=True)
    var = jnp.mean(jnp.square(grouped - mean), axis=-1, keepdims=True)
    scaled = (grouped - mean) * lax.rsqrt(var + group_eps) * small[-1].reshape(2, ch)
    activated = jax.nn.silu(scaled).astype(bf16)

    back = [activated[0]] + [shift_z(activated[1 + i], -d) for i, d in enumerate(SHIFTS)]
    by_shift = {0: back[0], **{d: back[1 + i] for i, d in enumerate(SHIFTS)}}
    relative = jnp.stack([by_shift[d] for d in range(4)])
    relative = jnp.concatenate([relative, relative], axis=0)
    ordered = lax.dynamic_slice_in_dim(relative, (4 - z) % 4, 4, axis=0)
    act = jnp.transpose(ordered, (2, 1, 0, 3)).reshape(2, rows, 4 * ch)
    mixed = dot_t(act[0], outw).astype(bf16).astype(f32) + dot_t(act[1], outw_other).astype(bf16).astype(f32)
    middle = (residual + mixed).astype(bf16)
    middle_f = middle.astype(f32)
    normed_ffn = rms_scale(middle_f, ffn_gain).astype(bf16)
    ffn_all = jnp.concatenate([normed_ffn] + [shift_z(normed_ffn, d) for d in SHIFTS], axis=0)

    ff = ffn_gate_weight.shape[1] // 4

    def hidden_of(w):
        both = dot(ffn_all, w)
        return (jax.nn.silu(both[:, :ff]) * both[:, ff:]).astype(bf16)

    part = dot_t(hidden_of(gu), down) + dot_t(hidden_of(gu_other), down_other)
    part = part.reshape(4, rows, width)
    fed = part[0]
    for i, d in enumerate(SHIFTS):
        fed = fed + shift_z(part[1 + i].astype(bf16), -d).astype(f32)
    return (middle_f + fed).astype(bf16).reshape(tokens.shape)


def solution(mesh):
    fine = Mesh(mesh.devices.reshape(2, 2, 4, 4, 2), ("zh", "zl", "y", "x", "tp"))
    wide = P(FS, "tp")
    seqs = P("tp", ("zh", "zl", "y", "x"), None)
    placed = (
        seqs,
        P(),
        wide,
        wide,
        P(None, "tp"),
        P("tp"),
        P("tp", FS),
        P(),
        wide,
        wide,
        P("tp", FS),
    )
    return jax.shard_map(body, mesh=fine, in_specs=placed, out_specs=seqs, check_vma=False)
```

```python
import jax
import jax.numpy as jnp
from jax import lax
from jax.experimental import pallas as pl
from jax.experimental.pallas import tpu as pltpu
from jax.sharding import Mesh, PartitionSpec as P


HALO = 16
norm_eps = 1e-06
group_eps = 1e-05

Z = ("zh", "zl")
FS = ("zl", "y", "x")
SHIFTS = (1, 3, 2)
f32 = jnp.float32
bf16 = jnp.bfloat16
VMEM_LIMIT = 48 * 1024 * 1024


def swap(value, axis):
    return lax.ppermute(value, axis, [(0, 1), (1, 0)])


def shift_z(value, by):
    return lax.ppermute(value, Z, [(i, (i + by) % 4) for i in range(4)])


def ring(value, axis):
    got = [value]
    for d in SHIFTS:
        got.append(lax.ppermute(value, axis, [(i, (i + d) % 4) for i in range(4)]))
    return got


def two_ways(pair):
    along_x = jnp.stack(ring(pair[0], "x"))
    along_y = jnp.stack(ring(pair[1], "y"))
    return ring(along_x, "y"), ring(along_y, "x")


def ordered(first, second, widths):
    offs = (0, *SHIFTS)
    me = jnp.stack([lax.axis_index("y"), lax.axis_index("x")]).astype(jnp.int32)
    n = len(widths)

    def kernel(at, *refs):
        src, out, sem = refs[:8], refs[8 : 8 + n], refs[-1]
        copies = []
        for jy in range(4):
            y = lax.rem(at[0] + 4 - offs[jy], 4)
            for jx in range(4):
                x = lax.rem(at[1] + 4 - offs[jx], 4)
                for zl, ref in ((0, src[jy].at[jx]), (1, src[4 + jx].at[jy])):
                    start = 0
                    for k, w in enumerate(widths):
                        copies.append(
                            pltpu.make_async_copy(
                                ref.at[:, start : start + w], out[k].at[zl, y, x], sem.at[len(copies)]
                            )
                        )
                        copies[-1].start()
                        start += w
        for copy in copies:
            copy.wait()

    return pl.pallas_call(
        kernel,
        out_shape=[jax.ShapeDtypeStruct((2, 4, 4, 64, w), bf16) for w in widths],
        in_specs=[pl.BlockSpec(memory_space=pltpu.SMEM)] + [pl.BlockSpec(memory_space=pltpu.HBM)] * 8,
        out_specs=[pl.BlockSpec(memory_space=pltpu.VMEM)] * n,
        scratch_shapes=[pltpu.SemaphoreType.DMA((32 * n,))],
        cost_estimate=pl.CostEstimate(flops=1 << 30, transcendentals=0, bytes_accessed=1 << 22),
        compiler_params=pltpu.CompilerParams(vmem_limit_bytes=VMEM_LIMIT),
    )(me, *first, *second)


def mm(a, b):
    return jnp.dot(a, b, preferred_element_type=f32)


def mm_t(a, b):
    return lax.dot_general(a, b, (((1,), (1,)), ((), ())), preferred_element_type=f32)


def whole_call(kernel, outs, args, scratch=(), flops=0):
    specs = [
        pl.BlockSpec(memory_space=pltpu.SMEM) if a.dtype == jnp.int32 else pl.BlockSpec(memory_space=pltpu.VMEM)
        for a in args
    ]
    out_specs = [pl.BlockSpec(memory_space=pltpu.VMEM) for _ in outs]
    return pl.pallas_call(
        kernel,
        out_shape=[jax.ShapeDtypeStruct(s, d) for s, d in outs],
        in_specs=specs,
        out_specs=out_specs,
        scratch_shapes=list(scratch),
        cost_estimate=pl.CostEstimate(flops=flops, transcendentals=0, bytes_accessed=1 << 20),
        compiler_params=pltpu.CompilerParams(vmem_limit_bytes=VMEM_LIMIT),
    )(*args)


def k_blocks():
    return [(zl, y, zl * 1024 + y * 256) for zl in range(2) for y in range(4)]


def times_rows(x, w_ref):
    cols = w_ref.shape[-1]
    acc = jnp.zeros((x.shape[0], cols), f32)
    for zl, y, at in k_blocks():
        acc = acc + mm(x[:, at : at + 256], w_ref[zl, y].reshape(256, cols))
    return acc


def glu_kernel(x0, x1, x2, x3, gain, wa, wb, out):
    for i, x in enumerate((x0, x1, x2, x3)):
        rows = x[...].astype(f32)
        scale = lax.rsqrt(jnp.mean(rows * rows, axis=-1, keepdims=True) + norm_eps)
        normed = (rows * scale * gain[...]).astype(bf16)
        for j, w in enumerate((wa, wb)):
            both = times_rows(normed, w)
            half = both.shape[1] // 2
            out[i, :, j * half : (j + 1) * half] = (both[:, :half] * jax.nn.sigmoid(both[:, half:])).astype(bf16)


def conv_kernel(tp, glu, edge, small, out, pad):
    seqs, rows, chans = glu.shape
    half = chans // 2
    taps = small.shape[0] - 1
    left = jnp.where(tp[0] == 1, 1.0, 0.0).astype(f32)
    right = 1.0 - left
    chunk = 32

    def one(s, carry):
        near = edge[s].astype(f32)
        near = jnp.concatenate([near[:, half:], near[:, :half]], axis=1)
        pad[0:HALO] = near * left
        pad[HALO : HALO + rows] = glu[s].astype(f32)
        pad[HALO + rows :] = near * right
        for c in range(2):
            lanes = slice(c * half, (c + 1) * half)
            gain = small[taps : taps + 1, lanes]
            for r in range(0, rows, chunk):
                acc = jnp.zeros((chunk, half), f32)
                for k in range(taps):
                    at = r + k + HALO - taps // 2
                    acc = acc + small[k : k + 1, lanes] * pad[at : at + chunk, lanes]
                mean = jnp.mean(acc, axis=-1, keepdims=True)
                off = acc - mean
                var = jnp.mean(off * off, axis=-1, keepdims=True)
                scaled = off * lax.rsqrt(var + group_eps) * gain
                out[s, r : r + chunk, lanes] = (scaled * jax.nn.sigmoid(scaled)).astype(bf16)
        return carry

    lax.fori_loop(0, seqs, one, 0)


def mix_kernel(z, a0, a1, a2, a3, wa, wb, tok, gain, middle, normed, act, mid):
    quarter = a0.shape[1] // 2
    for d, a in enumerate((a0, a1, a2, a3)):
        at = pl.multiple_of(lax.rem(z[0] + d, 4) * quarter, quarter)
        act[0, :, pl.ds(at, quarter)] = a[:, :quarter]
        act[1, :, pl.ds(at, quarter)] = a[:, quarter:]
    inner = wa.shape[-1]
    square = jnp.zeros((tok.shape[0], 128), f32)
    for zl, y, at in k_blocks():
        one = mm_t(act[0], wa[zl, y].reshape(256, inner)).astype(bf16).astype(f32)
        two = mm_t(act[1], wb[zl, y].reshape(256, inner)).astype(bf16).astype(f32)
        m = (tok[:, at : at + 256].astype(f32) + (one + two)).astype(bf16)
        middle[:, at : at + 256] = m
        m = m.astype(f32)
        mid[:, at : at + 256] = m
        square = square + m[:, :128] * m[:, :128] + m[:, 128:] * m[:, 128:]
    width = tok.shape[1]
    scale = lax.rsqrt(jnp.sum(square, axis=-1, keepdims=True) * (1.0 / width) + norm_eps)
    normed[...] = (mid[...] * scale * gain[...]).astype(bf16)


def ffn_kernel(x, ga, gb, da, db, out):
    hidden = []
    for w in (ga, gb):
        both = times_rows(x, w)
        half = both.shape[1] // 2
        gate = both[:, :half]
        hidden.append((gate * jax.nn.sigmoid(gate) * both[:, half:]).astype(bf16))
    inner = da.shape[-1]
    for zl, y, at in k_blocks():
        part = mm_t(hidden[0], da[zl, y].reshape(256, inner))
        part = part + mm_t(hidden[1], db[zl, y].reshape(256, inner))
        out[:, at : at + 256] = part.astype(out.dtype)


def layer(
    tokens,
    mix_gain,
    value_weight,
    gate_weight,
    conv_taps,
    head_gain,
    out_weight,
    ffn_gain,
    ffn_gate_weight,
    ffn_up_weight,
    down_weight,
):
    rows, _, width = tokens.shape
    zh, zl = lax.axis_index("zh"), lax.axis_index("zl")
    z = 2 * zh + zl
    tp = lax.axis_index("tp")
    ch = value_weight.shape[1] // 4

    def quarter(weight, of):
        size = weight.shape[1] // 4
        return lax.dynamic_slice_in_dim(weight, of * size, size, axis=1)

    def mine_theirs(*weights):
        return tuple(
            jnp.concatenate([quarter(w, of) for w in weights], axis=1) for of in (z, 2 * zh + 1 - zl)
        )

    def paired(mine, theirs):
        got = swap(theirs, "zl")
        return jnp.where(zl == 0, mine, got), jnp.where(zl == 0, got, mine)

    tok2 = tokens.reshape(rows, width)
    vg_mine, vg_theirs = mine_theirs(value_weight, gate_weight)
    vg_cols = vg_mine.shape[1]
    out_mine = out_weight.T
    out_cols = out_mine.shape[1]
    pair = paired(jnp.concatenate([vg_mine, out_mine], axis=1), jnp.concatenate([vg_theirs, out_mine], axis=1))
    vg, outw = ordered(*two_ways(pair), (vg_cols, out_cols))

    xs = ring(tok2, Z)

    gu_mine, gu_theirs = mine_theirs(ffn_gate_weight, ffn_up_weight)
    dn_mine, dn_theirs = mine_theirs(down_weight.T)
    gu_cols, dn_cols = gu_mine.shape[1], dn_mine.shape[1]
    pair = paired(jnp.concatenate([gu_mine, dn_mine], axis=1), jnp.concatenate([gu_theirs, dn_theirs], axis=1))
    gu, down = ordered(*two_ways(pair), (gu_cols, dn_cols))

    small = jnp.concatenate([conv_taps, head_gain[None]], axis=0)
    small = lax.dynamic_slice_in_dim(small, z * ch, ch, axis=1)
    small = jnp.concatenate([small, swap(small, "tp")], axis=1)

    (glu,) = whole_call(
        glu_kernel,
        [((4, rows, 2 * ch), bf16)],
        [*xs, mix_gain.reshape(1, width), vg, swap(vg, "tp")],
        flops=4 * rows * width * 4 * ch * 2,
    )
    edge = lax.dynamic_slice_in_dim(glu, jnp.where(tp == 0, rows - HALO, 0), HALO, axis=1)
    edge = swap(edge, "tp")
    (activated,) = whole_call(
        conv_kernel,
        [((4, rows, 2 * ch), bf16)],
        [tp.astype(jnp.int32).reshape(1), glu, edge, small],
        scratch=[pltpu.VMEM((rows + 2 * HALO, 2 * ch), f32)],
        flops=4 * rows * 2 * ch * 64,
    )
    back = {0: activated[0], **{d: shift_z(activated[1 + i], -d) for i, d in enumerate(SHIFTS)}}
    middle, normed_ffn = whole_call(
        mix_kernel,
        [((rows, width), bf16), ((rows, width), bf16)],
        [
            z.astype(jnp.int32).reshape(1),
            *[back[d] for d in range(4)],
            outw,
            swap(outw, "tp"),
            tok2,
            ffn_gain.reshape(1, width),
        ],
        scratch=[pltpu.VMEM((2, rows, 4 * ch), bf16), pltpu.VMEM((rows, width), f32)],
        flops=rows * width * 8 * ch * 2,
    )
    gu_other, down_other = swap(gu, "tp"), swap(down, "tp")
    far = [shift_z(normed_ffn, d) for d in SHIFTS]
    ff_flops = rows * width * gu_cols * 6

    def piece(x, kind):
        (out,) = whole_call(ffn_kernel, [((rows, width), kind)], [x, gu, gu_other, down, down_other], flops=ff_flops)
        return out

    returned = [shift_z(piece(x, bf16), -d) for x, d in zip(far, SHIFTS)]
    fed = piece(normed_ffn, f32)
    for part in returned:
        fed = fed + part.astype(f32)
    return (middle.astype(f32) + fed).astype(bf16).reshape(tokens.shape)


def solution(mesh):
    fine = Mesh(mesh.devices.reshape(2, 2, 4, 4, 2), ("zh", "zl", "y", "x", "tp"))
    wide = P(FS, "tp")
    seqs = P("tp", ("zh", "zl", "y", "x"), None)
    placed = (
        seqs,
        P(),
        wide,
        wide,
        P(None, "tp"),
        P("tp"),
        P("tp", FS),
        P(),
        wide,
        wide,
        P("tp", FS),
    )
    return jax.shard_map(layer, mesh=fine, in_specs=placed, out_specs=seqs, check_vma=False)
```

```python
import jax
import jax.numpy as jnp
from jax import lax
from jax.experimental import pallas as pl
from jax.experimental.pallas import tpu as pltpu
from jax.sharding import Mesh, PartitionSpec as P


HALO = 16
norm_eps = 1e-06
group_eps = 1e-05

Z = ("zh", "zl")
FS = ("zl", "y", "x")
SHIFTS = (1, 3, 2)
f32 = jnp.float32
bf16 = jnp.bfloat16
VMEM_LIMIT = 20 * 1024 * 1024


def swap(value, axis):
    return lax.ppermute(value, axis, [(0, 1), (1, 0)])


def shift_z(value, by):
    return lax.ppermute(value, Z, [(i, (i + by) % 4) for i in range(4)])


def ring(value, axis):
    got = [value]
    for d in SHIFTS:
        got.append(lax.ppermute(value, axis, [(i, (i + d) % 4) for i in range(4)]))
    return got


def ordered(groups, widths):
    offs = (0, *SHIFTS)
    me = jnp.stack([lax.axis_index(a) for a in ("y", "x", "zl")]).astype(jnp.int32)
    n = len(widths)
    pieces = [p for first, second in groups for p in (*first, *second)]

    def kernel(at, *refs):
        for g in range(len(groups)):
            src = refs[8 * g : 8 * g + 8]
            out = refs[len(pieces) + n * g : len(pieces) + n * g + n]
            for jy in range(4):
                y = lax.rem(at[0] + 4 - offs[jy], 4)
                for jx in range(4):
                    x = lax.rem(at[1] + 4 - offs[jx], 4)
                    for zl, block in ((at[2], src[jy].at[jx]), (1 - at[2], src[4 + jx].at[jy])):
                        start = 0
                        for k, w in enumerate(widths):
                            out[k][zl, y, x] = block[:, start : start + w]
                            start += w

    return whole_call(kernel, [((2, 4, 4, 64, w), bf16) for _ in groups for w in widths], [me, *pieces], flops=1 << 30)


def mm(a, b):
    return jnp.dot(a, b, preferred_element_type=f32)


def mm_t(a, b):
    return lax.dot_general(a, b, (((1,), (1,)), ((), ())), preferred_element_type=f32)


def whole_call(kernel, outs, args, scratch=(), flops=0, space=pltpu.VMEM):
    specs = [pl.BlockSpec(memory_space=pltpu.SMEM if a.dtype == jnp.int32 else space) for a in args]
    out_specs = [pl.BlockSpec(memory_space=pltpu.VMEM) for _ in outs]
    return pl.pallas_call(
        kernel,
        out_shape=[jax.ShapeDtypeStruct(s, d) for s, d in outs],
        in_specs=specs,
        out_specs=out_specs,
        scratch_shapes=list(scratch),
        cost_estimate=pl.CostEstimate(flops=flops, transcendentals=0, bytes_accessed=1 << 20),
        compiler_params=pltpu.CompilerParams(vmem_limit_bytes=VMEM_LIMIT),
    )(*args)


def k_blocks():
    return [(zl, y, zl * 1024 + y * 256) for zl in range(2) for y in range(4)]


def rows_of(w, start=0, stop=None):
    return w[..., start:stop].reshape(-1, (stop or w.shape[-1]) - start)


def glu_kernel(x0, x1, x2, x3, gain, wa, wb, out):
    for i, x in enumerate((x0, x1, x2, x3)):
        rows = x[...].astype(f32)
        scale = lax.rsqrt(jnp.mean(rows * rows, axis=-1, keepdims=True) + norm_eps)
        normed = (rows * scale * gain[...]).astype(bf16)
        for j, w in enumerate((wa, wb)):
            both = mm(normed, rows_of(w))
            half = both.shape[1] // 2
            out[i, :, j * half : (j + 1) * half] = (both[:, :half] * jax.nn.sigmoid(both[:, half:])).astype(bf16)


def conv_kernel(tp, glu, edge, small, out, pad):
    seqs, rows, chans = glu.shape
    half = chans // 2
    taps = small.shape[0] - 1
    left = jnp.where(tp[0] == 1, 1.0, 0.0).astype(f32)
    right = 1.0 - left
    chunk = rows

    def one(s, carry):
        near = edge[s].astype(f32)
        near = jnp.concatenate([near[:, half:], near[:, :half]], axis=1)
        pad[0:HALO] = near * left
        pad[HALO : HALO + rows] = glu[s].astype(f32)
        pad[HALO + rows :] = near * right
        for c in range(2):
            lanes = slice(c * half, (c + 1) * half)
            gain = small[taps : taps + 1, lanes]
            for r in range(0, rows, chunk):
                acc = jnp.zeros((chunk, half), f32)
                for k in range(taps):
                    at = r + k + HALO - taps // 2
                    acc = acc + small[k : k + 1, lanes] * pad[at : at + chunk, lanes]
                mean = jnp.mean(acc, axis=-1, keepdims=True)
                off = acc - mean
                var = jnp.mean(off * off, axis=-1, keepdims=True)
                scaled = off * lax.rsqrt(var + group_eps) * gain
                out[s, r : r + chunk, lanes] = (scaled * jax.nn.sigmoid(scaled)).astype(bf16)
        return carry

    lax.fori_loop(0, seqs, one, 0)


def mix_kernel(z, a0, a1, a2, a3, wa, wb, tok, gain, middle, normed, act, mid):
    quarter = a0.shape[1] // 2
    for d, a in enumerate((a0, a1, a2, a3)):
        at = pl.multiple_of(lax.rem(z[0] + d, 4) * quarter, quarter)
        act[0, :, pl.ds(at, quarter)] = a[:, :quarter]
        act[1, :, pl.ds(at, quarter)] = a[:, quarter:]
    inner = wa.shape[-1]
    square = jnp.zeros((tok.shape[0], 128), f32)
    for zl, y, at in k_blocks():
        one = mm_t(act[0], wa[zl, y].reshape(256, inner)).astype(bf16).astype(f32)
        two = mm_t(act[1], wb[zl, y].reshape(256, inner)).astype(bf16).astype(f32)
        m = (tok[:, at : at + 256].astype(f32) + (one + two)).astype(bf16)
        middle[:, at : at + 256] = m
        m = m.astype(f32)
        mid[:, at : at + 256] = m
        square = square + m[:, :128] * m[:, :128] + m[:, 128:] * m[:, 128:]
    width = tok.shape[1]
    scale = lax.rsqrt(jnp.sum(square, axis=-1, keepdims=True) * (1.0 / width) + norm_eps)
    normed[...] = (mid[...] * scale * gain[...]).astype(bf16)


def ffn_kernel(*refs):
    *xs, wa, wb, out = refs
    x = xs[0][...] if len(xs) == 1 else jnp.concatenate([part[...] for part in xs], axis=0)
    ff = wa.shape[-1] // 3
    part = None
    for w in (wa, wb):
        both = mm(x, rows_of(w, 0, 2 * ff))
        gate = both[:, :ff]
        hidden = (gate * jax.nn.sigmoid(gate) * both[:, ff:]).astype(bf16)
        one = mm_t(hidden, rows_of(w, 2 * ff, 3 * ff))
        part = one if part is None else part + one
    out[...] = part.astype(out.dtype)


def prep_kernel(at, value, gate, outw, ffn_gate, ffn_up, down, mine, theirs, sem):
    copies = []
    for which, out in enumerate((mine, theirs)):
        start = 0
        for w in (value, gate, outw, ffn_gate, ffn_up, down):
            if w is outw:
                size = w.shape[1]
                src = w
            else:
                size = w.shape[1] // 4
                src = w.at[:, pl.ds(pl.multiple_of(at[which] * size, 128), size)]
            copies.append(pltpu.make_async_copy(src, out.at[:, start : start + size], sem.at[len(copies)]))
            copies[-1].start()
            start += size
    for copy in copies:
        copy.wait()


def layer(
    tokens,
    mix_gain,
    value_weight,
    gate_weight,
    conv_taps,
    head_gain,
    out_weight,
    ffn_gain,
    ffn_gate_weight,
    ffn_up_weight,
    down_weight,
):
    rows, _, width = tokens.shape
    zh, zl = lax.axis_index("zh"), lax.axis_index("zl")
    z = 2 * zh + zl
    tp = lax.axis_index("tp")
    ch = value_weight.shape[1] // 4

    tok2 = tokens.reshape(rows, width)
    vg_cols, out_cols = 2 * ch, out_weight.shape[0]
    gu_cols, dn_cols = ffn_gate_weight.shape[1] // 2, down_weight.shape[0] // 4
    shards = [value_weight, gate_weight, out_weight.T, ffn_gate_weight, ffn_up_weight, down_weight.T]
    cols = vg_cols + out_cols + gu_cols + dn_cols
    shard_rows = value_weight.shape[0]
    mine, theirs = whole_call(
        prep_kernel,
        [((shard_rows, cols), bf16)] * 2,
        [
            jnp.stack([z, 2 * zh + 1 - zl]).astype(jnp.int32),
            *[pltpu.with_memory_space_constraint(w, pltpu.HBM) for w in shards],
        ],
        scratch=[pltpu.SemaphoreType.DMA((12,))],
        flops=1 << 20,
        space=pltpu.HBM,
    )
    along_x = ring(mine, "x")
    along_y = ring(swap(theirs, "zl"), "y")

    def second(start, size):
        cut = lambda pieces: jnp.stack([lax.slice_in_dim(p, start, start + size, axis=1) for p in pieces])
        return ring(cut(along_x), "y"), ring(cut(along_y), "x")

    split = vg_cols + out_cols
    vg, outw = ordered([second(0, split)], (vg_cols, out_cols))
    first, last = second(split, cols - split)
    others = [[swap(p, "tp") for p in side] for side in (first, last)]
    ffn_own, ffn_other = ordered([(first, last), others], (cols - split,))
    xs = ring(tok2, Z)

    small = jnp.concatenate([conv_taps, head_gain[None]], axis=0)
    small = lax.dynamic_slice_in_dim(small, z * ch, ch, axis=1)
    small = jnp.concatenate([small, swap(small, "tp")], axis=1)

    (glu,) = whole_call(
        glu_kernel,
        [((4, rows, 2 * ch), bf16)],
        [*xs, mix_gain.reshape(1, width), vg, swap(vg, "tp")],
        flops=4 * rows * width * 4 * ch * 2,
    )
    edge = lax.dynamic_slice_in_dim(glu, jnp.where(tp == 0, rows - HALO, 0), HALO, axis=1)
    edge = swap(edge, "tp")
    (activated,) = whole_call(
        conv_kernel,
        [((4, rows, 2 * ch), bf16)],
        [tp.astype(jnp.int32).reshape(1), glu, edge, small],
        scratch=[pltpu.VMEM((rows + 2 * HALO, 2 * ch), f32)],
        flops=4 * rows * 2 * ch * 64,
    )
    back = {0: activated[0], **{d: shift_z(activated[1 + i], -d) for i, d in enumerate(SHIFTS)}}
    middle, normed_ffn = whole_call(
        mix_kernel,
        [((rows, width), bf16), ((rows, width), bf16)],
        [
            z.astype(jnp.int32).reshape(1),
            *[back[d] for d in range(4)],
            outw,
            swap(outw, "tp"),
            tok2,
            ffn_gain.reshape(1, width),
        ],
        scratch=[pltpu.VMEM((2, rows, 4 * ch), bf16), pltpu.VMEM((rows, width), f32)],
        flops=rows * width * 8 * ch * 2,
    )
    half = rows // 2
    below = shift_z(normed_ffn, 1)
    above = shift_z(normed_ffn, 3)
    opposite = (shift_z(above[:half], 3), shift_z(below[half:], 1))
    ff_flops = rows * width * gu_cols * 6

    def piece(xs, kind):
        (out,) = whole_call(ffn_kernel, [((rows, width), kind)], [*xs, ffn_own, ffn_other], flops=ff_flops)
        return out

    returned = [shift_z(piece(xs, bf16), -d) for xs, d in (((below,), 1), ((above,), 3), (opposite, 2))]
    fed = piece((normed_ffn,), f32)
    for part in returned:
        fed = fed + part.astype(f32)
    return (middle.astype(f32) + fed).astype(bf16).reshape(tokens.shape)


def solution(mesh):
    fine = Mesh(mesh.devices.reshape(2, 2, 4, 4, 2), ("zh", "zl", "y", "x", "tp"))
    wide = P(FS, "tp")
    seqs = P("tp", ("zh", "zl", "y", "x"), None)
    placed = (
        seqs,
        P(),
        wide,
        wide,
        P(None, "tp"),
        P("tp"),
        P("tp", FS),
        P(),
        wide,
        wide,
        P("tp", FS),
    )
    return jax.shard_map(layer, mesh=fine, in_specs=placed, out_specs=seqs, check_vma=False)
```
